32 devices in a mesh: rep: 2 (over x), fs: 8 (over z, y), tp: 2 (over core).
Axes of the slice: x: 2, y: 2, z: 4, core: 2. Of those that a mesh axis runs over, the one named last changes fastest.
Arguments:
- tokens: bfloat16 [6144, 2048], P(('rep', 'fs', 'tp')), may hold values from -6 to 6
- mix_gain_in: float32 [2048], replicated, may hold values from 0.1 to 1.9
- pool_weight: bfloat16 [4, 512, 512], P(None, 'fs'), may hold values from -0.25 to 0.25
- mix_gain_out: float32 [2048], replicated, may hold values from 0.1 to 1.9
- ffn_gain_in: float32 [2048], replicated, may hold values from 0.1 to 1.9
- gate_weight: bfloat16 [2048, 5632], P('fs', 'tp'), may hold values from -0.125 to 0.125
- up_weight: bfloat16 [2048, 5632], P('fs', 'tp'), may hold values from -0.125 to 0.125
- gate_taps: float32 [3, 5632], replicated, may hold values from -3.5 to 3.5
- up_taps: float32 [3, 5632], replicated, may hold values from -3.5 to 3.5
- down_weight: bfloat16 [5632, 2048], P('tp', 'fs'), may hold values from -0.078125 to 0.078125
- ffn_gain_out: float32 [2048], replicated, may hold values from 0.1 to 1.9
Outputs:
- mixed_out: bfloat16 [6144, 2048], P(('rep', 'fs', 'tp'))
The draws below stay inside these ranges and needn't reach their ends.
All inputs are finite; a program needn't handle non-finite values.
Results may differ from the reference program's by a relative error of at most 0.014.
Values may be sent and summed in bfloat16 or wider, within the bound.
A program may use at most 128 MiB of HBM per device.

```python
import jax
import jax.numpy as jnp
from jax import lax

D = 2048
FF = 5632
GROUPS = 4
CONV_WIDTH = 3
GC = 512
SEQ_LEN = 384
SEQS = 16
TOKENS = 6144
N_TP = 2


def level_of(rng, dims, cuts, smallest, largest):
    level = 1.0
    for position, blocks in cuts:
        heights = jax.random.uniform(jax.random.fold_in(jax.random.fold_in(rng, 6), position), (blocks,), jnp.float32, smallest / len(cuts), largest / len(cuts))
        level = level * jnp.repeat(jnp.exp(heights), dims[position] // blocks).reshape((-1,) + (1,) * (len(dims) - 1 - position))
    return level


def bell_draw(own_key, dims, deviation, limit, cuts=(), kind=jnp.bfloat16):
    values = jax.random.normal(own_key, dims, jnp.float32) * deviation
    if len(cuts) > 0:
        values = level_of(own_key, dims, cuts, -0.22, 0.18) * values
    return jnp.clip(values, min=-limit, max=limit).astype(kind)


def setup_inputs(seed: int = 0) -> dict:
    key_of = jax.random.split(jax.random.key(seed), 12)
    return {
        "tokens": bell_draw(key_of[0], (TOKENS, D), 1.0, 6.0, ((0, 32),)),
        "mix_gain_in": jnp.clip(1.0 + 0.18 * jax.random.normal(key_of[1], (D,), jnp.float32), 0.1, 1.9),
        "pool_weight": bell_draw(key_of[2], (GROUPS, GC, GC), GC ** -0.5, 0.25, ((1, 8),)),
        "mix_gain_out": jnp.clip(1.0 + 0.18 * jax.random.normal(key_of[3], (D,), jnp.float32), 0.1, 1.9),
        "ffn_gain_in": jnp.clip(1.0 + 0.18 * jax.random.normal(key_of[4], (D,), jnp.float32), 0.1, 1.9),
        "gate_weight": bell_draw(key_of[5], (D, FF), D ** -0.5, 0.125, ((0, 8), (1, 2))),
        "up_weight": bell_draw(key_of[6], (D, FF), D ** -0.5, 0.125, ((0, 8), (1, 2))),
        "gate_taps": bell_draw(key_of[7], (CONV_WIDTH, FF), CONV_WIDTH ** -0.5, 3.5, (), jnp.float32),
        "up_taps": bell_draw(key_of[8], (CONV_WIDTH, FF), CONV_WIDTH ** -0.5, 3.5, (), jnp.float32),
        "down_weight": bell_draw(key_of[9], (FF, D), FF ** -0.5, 0.078125, ((0, 2), (1, 8))),
        "ffn_gain_out": jnp.clip(1.0 + 0.18 * jax.random.normal(key_of[10], (D,), jnp.float32), 0.1, 1.9),
    }


pool_spans = (2, 4, 8, 16)
rms_eps = 1e-06

def rms_scale(values, gain):
    floats = values.astype(jnp.float32)
    return floats * lax.rsqrt(lax.optimization_barrier(jnp.mean(floats * floats, axis=-1, keepdims=True)) + rms_eps) * gain.astype(jnp.float32)

def pooled_gap(padded, first, count):
    margin = padded.shape[0] - count
    floats = padded.astype(jnp.float32)
    width = padded.shape[1] // len(pool_spans)
    where = first + jnp.arange(count, dtype=jnp.int32)
    pieces = []
    for group, span in enumerate(pool_spans):
        block = floats[:, group * width:(group + 1) * width]
        total = jnp.zeros((count, width), jnp.float32)
        for back in range(span):
            total = total + block[margin - back:margin - back + count]
        divisor = jnp.minimum(where + 1, span).astype(jnp.float32)
        pieces.append(total / divisor[:, None] - block[margin:])
    return jnp.concatenate(pieces, axis=1).astype(jnp.bfloat16)

def causal_taps(pre, taps):
    width = taps.shape[0]
    floats = pre.astype(jnp.float32)
    padded = jnp.concatenate([jnp.zeros((width - 1, pre.shape[1]), jnp.float32), floats], axis=0)
    total = jnp.zeros(floats.shape, jnp.float32)
    for offset in range(width):
        total = total + taps[offset].astype(jnp.float32) * padded[offset:offset + pre.shape[0]]
    return total

def reference(tokens, mix_gain_in, pool_weight, mix_gain_out, ffn_gain_in, gate_weight, up_weight, gate_taps, up_taps, down_weight, ffn_gain_out):
    margin = max(pool_spans) - 1

    def one_sequence(rows):
        normed = rms_scale(rows, mix_gain_in).astype(jnp.bfloat16)
        padded = jnp.concatenate([jnp.zeros((margin, D), jnp.bfloat16), normed], axis=0)
        gap = pooled_gap(padded, 0, SEQ_LEN)
        mixed = jnp.einsum('rgc,gcj->rgj', gap.reshape(SEQ_LEN, GROUPS, GC).astype(jnp.float32), pool_weight.astype(jnp.float32))
        mixed = mixed.reshape(SEQ_LEN, D).astype(jnp.bfloat16)
        after_mix = rows.astype(jnp.float32) + rms_scale(mixed, mix_gain_out)
        channel_in = rms_scale(after_mix, ffn_gain_in).astype(jnp.bfloat16)
        gate_pre = jnp.dot(channel_in, gate_weight, preferred_element_type=jnp.float32).astype(jnp.bfloat16)
        up_pre = jnp.dot(channel_in, up_weight, preferred_element_type=jnp.float32).astype(jnp.bfloat16)
        gate_conv = causal_taps(gate_pre, gate_taps)
        up_conv = causal_taps(up_pre, up_taps)
        hidden = (jax.nn.gelu(gate_conv, approximate=True) * up_conv).astype(jnp.bfloat16)
        partial_value = jnp.einsum('rtf,tfd->rtd', hidden.reshape(SEQ_LEN, N_TP, FF // N_TP).astype(jnp.float32), down_weight.reshape(N_TP, FF // N_TP, D).astype(jnp.float32)).astype(jnp.bfloat16)
        channel_out = lax.optimization_barrier(jnp.sum(partial_value.astype(jnp.float32), axis=1))
        return (after_mix + rms_scale(channel_out, ffn_gain_out)).astype(jnp.bfloat16)
    result = lax.map(one_sequence, tokens.reshape(SEQS, SEQ_LEN, D))
    return result.reshape(TOKENS, D)
```

```python
import functools

import jax
import jax.numpy as jnp
from jax import lax
from jax.experimental import pallas as pl
from jax.experimental.pallas import tpu as pltpu
from jax.sharding import PartitionSpec as P

MESH = pl.DeviceIdType.MESH
pool_spans = (2, 4, 8, 16)
rms_eps = 1e-06
weight_budget = 24 * 2**20
f32 = jnp.float32
bf16 = jnp.bfloat16


def rms_scale(floats, gain):
    return floats * lax.rsqrt(jnp.mean(floats * floats, axis=-1, keepdims=True) + rms_eps) * gain


def gelu(v):
    return 0.5 * v * (1.0 + jnp.tanh(0.7978845608028654 * (v + 0.044715 * v * v * v)))


class Plan:
    def __init__(self, mesh, depth, width, columns):
        self.R, self.F, self.T = mesh.shape["rep"], mesh.shape["fs"], mesh.shape["tp"]
        self.Y = 1
        while 4 * self.Y * self.Y <= self.F:
            self.Y *= 2
        while self.F % self.Y:
            self.Y -= 1
        self.Z = self.F // self.Y
        self.joined = 3 * width * columns * 2 > weight_budget
        self.n_sub = self.R * self.Y if self.joined else 1
        self.G = self.T * self.n_sub
        self.cols = columns // self.n_sub


def kernel(
    plan, tokens, gain_in, pool, gain_out, gain_ffn, w, gate_taps, up_taps, gain_last, out,
    halo, pool_all, w_gu, w_d, x_all, normed, after, acc_g, acc_u, hidden, partial, got,
    own_sem, halo_sem, y_ss, up_ss, dn_ss, piece_rs, share_ss, share_rs, x_ss, x_rs, p_ss, p_rs,
):
    R, F, T, Y, Z, G, cols = plan.R, plan.F, plan.T, plan.Y, plan.Z, plan.G, plan.cols
    r, f, t = lax.axis_index("rep"), lax.axis_index("fs"), lax.axis_index("tp")
    z, y = f // Y, f % Y
    rows, width = tokens.shape
    depth = width // F
    groups, gc = pool_all.shape[0], pool_all.shape[1]
    slab = gc // F
    S = min(T, groups)
    GS = groups // S
    q = t % S
    margin = halo.shape[0]
    POOL, GU, DN = 0, 1, 2

    if plan.joined:
        me = (r * Y + y) * T + t
    else:
        me = t

    def member(g):
        if plan.joined:
            return {"rep": g // (T * Y), "fs": z * Y + (g // T) % Y, "tp": g % T}
        return {"tp": g}

    def sub_of(y_to):
        return r * Y + y_to if plan.joined else 0

    def w_rows(y_to):
        return pl.ds(pl.multiple_of(sub_of(y_to) * cols, 64 if cols % 64 == 0 else 8), cols)

    def slot(kind, origin):
        if kind == POOL:
            return pool_all.at[pl.ds(q * GS, GS), pl.ds(pl.multiple_of(origin * slab, slab), slab)]
        return w_gu.at[origin] if kind == GU else w_d.at[origin]

    def source(kind, y_to):
        if kind == POOL:
            return pool.at[pl.ds(q * GS, GS)]
        if kind == GU:
            return w.at[pl.ds(0, 2), w_rows(y_to)]
        return w.at[2, w_rows(y_to)]

    def own_copy(kind):
        return pltpu.make_async_copy(source(kind, y), slot(kind, f), own_sem.at[kind])

    def y_copy(kind, step):
        y_to = (y + step) % Y
        return pltpu.make_async_remote_copy(
            src_ref=source(kind, y_to), dst_ref=slot(kind, f), send_sem=y_ss.at[kind, step - 1],
            recv_sem=piece_rs.at[kind, f], device_id={"fs": z * Y + y_to}, device_id_type=MESH)

    def chain_copy(kind, origin, dz):
        return pltpu.make_async_remote_copy(
            src_ref=slot(kind, origin), dst_ref=slot(kind, origin), send_sem=(up_ss if dz > 0 else dn_ss).at[kind, origin],
            recv_sem=piece_rs.at[kind, origin], device_id={"fs": (z + dz) * Y + y}, device_id_type=MESH)

    def send_up(kind, origin):
        @pl.when(z + 1 < Z)
        def _():
            chain_copy(kind, origin, 1).start()

    def send_down(kind, origin):
        @pl.when(z > 0)
        def _():
            chain_copy(kind, origin, -1).start()

    def arrived(kind, origin):
        chain_copy(kind, origin, 1).wait_recv()

    def chain_plane(kind):
        own_copy(kind).wait()
        send_up(kind, f)
        send_down(kind, f)
        for step in range(1, Y):
            origin = z * Y + (y + step) % Y
            arrived(kind, origin)
            send_up(kind, origin)
            send_down(kind, origin)

    def chain_step(kind, s, use=None):
        for step in range(Y):
            @pl.when(z >= s)
            def _():
                origin = (z - s) * Y + (y + step) % Y
                arrived(kind, origin)
                send_up(kind, origin)

            @pl.when(z + s < Z)
            def _():
                origin = (z + s) * Y + (y + step) % Y
                arrived(kind, origin)
                send_down(kind, origin)
        if use is not None:
            use_step(s, use)

    def use_step(s, use):
        for sign in (-1, 1):
            @pl.when((z >= s) if sign < 0 else (z + s < Z))
            def _():
                def body(step, carry):
                    use((z + sign * s) * Y + (y + step) % Y)
                    return carry
                lax.fori_loop(0, Y, body, 0)

    def use_plane(use):
        def body(step, carry):
            use(z * Y + (y + step) % Y)
            return carry
        lax.fori_loop(0, Y, body, 0)

    def halo_copy():
        return pltpu.make_async_remote_copy(
            src_ref=tokens.at[pl.ds(rows - margin, margin)], dst_ref=halo, send_sem=halo_sem.at[0],
            recv_sem=halo_sem.at[1], device_id={"tp": (t + 1) % T}, device_id_type=MESH)

    def share_copy(step, q_from):
        return pltpu.make_async_remote_copy(
            src_ref=pool_all.at[pl.ds(q_from * GS, GS)], dst_ref=pool_all.at[pl.ds(q_from * GS, GS)],
            send_sem=share_ss.at[step - 1], recv_sem=share_rs.at[q_from],
            device_id={"tp": t - q + (q + step) % S}, device_id_type=MESH)

    def x_copy(step, g_from):
        return pltpu.make_async_remote_copy(
            src_ref=x_all.at[g_from], dst_ref=x_all.at[g_from], send_sem=x_ss.at[step - 1],
            recv_sem=x_rs.at[g_from], device_id=member((me + step) % G), device_id_type=MESH)

    def p_copy(step, block, g_from):
        g_to = (me + step) % G
        return pltpu.make_async_remote_copy(
            src_ref=partial.at[block, g_to], dst_ref=got.at[block, g_from], send_sem=p_ss.at[block, step - 1],
            recv_sem=p_rs.at[block, g_from], device_id=member(g_to), device_id_type=MESH)

    for kind in (POOL, GU, DN):
        own_copy(kind).start()
    halo_copy().start()
    for kind in (POOL, GU, DN):
        for step in range(1, Y):
            y_copy(kind, step).start()
    chain_plane(POOL)
    for s in range(1, Z):
        chain_step(POOL, s)
    chain_plane(GU)
    for step in range(1, S):
        share_copy(step, q).start()

    halo_copy().wait_recv()
    before = rms_scale(halo[...].astype(f32), gain_in[...]).astype(bf16).astype(f32)
    normed[pl.ds(0, margin), :] = jnp.where(t > 0, before, 0.0)
    normed[pl.ds(margin, rows), :] = rms_scale(tokens[...].astype(f32), gain_in[...]).astype(bf16).astype(f32)
    where = t * rows + lax.broadcasted_iota(jnp.int32, (rows, gc), 0)
    for step in range(1, S):
        share_copy(step, (q + step) % S).wait_recv()
    for group, span in enumerate(pool_spans):
        total = normed[:, group * gc : (group + 1) * gc]
        block = total[margin:]
        reach = 1
        while reach < span:
            total = total + pltpu.roll(total, reach, 0)
            reach *= 2
        gap = (total[margin:] / jnp.minimum(where + 1, span).astype(f32) - block).astype(bf16)
        mixed = jnp.dot(gap, pool_all[group], preferred_element_type=f32)
        after[:, group * gc : (group + 1) * gc] = mixed.astype(bf16).astype(f32)
    after[...] = tokens[...].astype(f32) + rms_scale(after[...], gain_out[...])
    whole = rms_scale(after[...], gain_ffn[...]).astype(bf16)
    for k in range(F):
        x_all[me, k] = whole[:, k * depth : (k + 1) * depth]
    for step in range(1, G):
        x_copy(step, me).start()

    acc_g[...] = jnp.zeros_like(acc_g)
    acc_u[...] = jnp.zeros_like(acc_u)

    def times(lhs, rhs):
        return lax.dot_general(lhs, rhs, (((1,), (1,)), ((), ())), preferred_element_type=f32)

    def gate_up(origin):
        def body(g, carry):
            x = x_all[g, origin]
            at = pl.ds(pl.multiple_of(8 + g * rows, 8), rows)
            acc_g[at, :] += times(x, w_gu[origin, 0])
            acc_u[at, :] += times(x, w_gu[origin, 1])
            return carry
        lax.fori_loop(0, G, body, 0)

    chain_step(GU, 1)
    chain_plane(DN)
    for step in range(1, G):
        x_copy(step, (me + step) % G).wait_recv()
    use_plane(gate_up)
    use_step(1, gate_up)
    for s in range(2, Z):
        chain_step(GU, s, gate_up)
    chain_step(DN, 1)

    taps = gate_taps.shape[0]

    def convolve(acc, taps_ref, g, keep):
        block = acc[pl.ds(pl.multiple_of(g * rows, 8), rows + 8), :]
        total = taps_ref[taps - 1 : taps, :] * block[8:]
        for back in range(1, taps):
            moved = pltpu.roll(block, back, 0)[8:]
            total = total + taps_ref[taps - 1 - back : taps - back, :] * jnp.where(keep >= back, moved, 0.0)
        return total

    def activate(g, carry):
        keep = (g % T) * rows + lax.broadcasted_iota(jnp.int32, (rows, cols), 0)
        hidden[g] = (gelu(convolve(acc_g, gate_taps, g, keep)) * convolve(acc_u, up_taps, g, keep)).astype(bf16)
        return carry

    lax.fori_loop(0, G, activate, 0)

    def down(block):
        def body(g, carry):
            partial[block, g] = jnp.dot(hidden[g], w_d[block], preferred_element_type=f32).astype(bf16)
            return carry
        lax.fori_loop(0, G, body, 0)
        for step in range(1, G):
            p_copy(step, block, me).start()
        got[block, me] = partial[block, me]

    use_plane(down)
    use_step(1, down)
    for s in range(2, Z):
        chain_step(DN, s, down)

    def finish(block, carry):
        for step in range(1, G):
            p_copy(step, block, (me + step) % G).wait_recv()
        return carry

    lax.fori_loop(0, F, finish, 0)
    for k in range(F):
        total = got[k, 0].astype(f32)
        for g in range(1, G):
            total = total + got[k, g].astype(f32)
        normed[pl.ds(0, rows), k * depth : (k + 1) * depth] = total
    out[...] = (after[...] + rms_scale(normed[pl.ds(0, rows), :], gain_last[...])).astype(bf16)

    halo_copy().wait_send()
    for step in range(1, S):
        share_copy(step, q).wait_send()
    for step in range(1, G):
        x_copy(step, me).wait_send()
    for kind in (POOL, GU, DN):
        for step in range(1, Y):
            y_copy(kind, step).wait_send()

        def ended(origin, carry):
            @pl.when((origin // Y <= z) & (z + 1 < Z))
            def _():
                chain_copy(kind, origin, 1).wait_send()

            @pl.when((origin // Y >= z) & (z > 0))
            def _():
                chain_copy(kind, origin, -1).wait_send()
            return carry
        lax.fori_loop(0, F, ended, 0)

    def sent(block, carry):
        for step in range(1, G):
            p_copy(step, block, me).wait_send()
        return carry
    lax.fori_loop(0, F, sent, 0)


def solution(mesh):
    def shards(tokens, gain_in, pool, gain_out, gain_ffn, gate_w, up_w, gate_taps, up_taps, down_w, gain_last):
        rows, width = tokens.shape
        depth, columns = gate_w.shape
        plan = Plan(mesh, depth, width, columns)
        F, G, T, Y, Z, cols = plan.F, plan.G, plan.T, plan.Y, plan.Z, plan.cols
        groups, gc = pool.shape[0], pool.shape[2]
        w = jnp.stack([gate_w.T, up_w.T, down_w])
        first = lax.axis_index("tp") * columns
        if plan.joined:
            first = first + (lax.axis_index("rep") * Y + lax.axis_index("fs") % Y) * cols
        gt = lax.dynamic_slice_in_dim(gate_taps, first, cols, 1)
        ut = lax.dynamic_slice_in_dim(up_taps, first, cols, 1)
        margin = max(pool_spans)
        vmem = pl.BlockSpec(memory_space=pltpu.VMEM)
        anywhere = pl.BlockSpec(memory_space=pl.ANY)
        dma = pltpu.SemaphoreType.DMA
        S = min(T, groups)
        V = pltpu.VMEM
        return pl.pallas_call(
            functools.partial(kernel, plan),
            out_shape=jax.ShapeDtypeStruct((rows, width), bf16),
            in_specs=[vmem, vmem, anywhere, vmem, vmem, anywhere, vmem, vmem, vmem],
            out_specs=vmem,
            scratch_shapes=[
                V((margin, width), bf16), V((groups, gc, gc), bf16), V((F, 2, cols, depth), bf16), V((F, cols, depth), bf16),
                V((G, F, rows, depth), bf16), V((margin + rows, width), f32), V((rows, width), f32),
                V((8 + G * rows, cols), f32), V((8 + G * rows, cols), f32), V((G, rows, cols), bf16),
                V((F, G, rows, depth), bf16), V((F, G, rows, depth), bf16),
                dma((3,)), dma((2,)), dma((3, max(Y - 1, 1))), dma((3, F)), dma((3, F)), dma((3, F)),
                dma((max(S - 1, 1),)), dma((S,)), dma((G - 1,)), dma((G,)), dma((F, G - 1)), dma((F, G)),
            ],
            compiler_params=pltpu.CompilerParams(has_side_effects=True, vmem_limit_bytes=61 * 2**20),
            name="layer",
        )(tokens, gain_in[None], pool, gain_out[None], gain_ffn[None], w, gt, ut, gain_last[None])

    in_specs = (
        P(("rep", "fs", "tp"), None), P(), P(None, "fs", None), P(), P(),
        P("fs", "tp"), P("fs", "tp"), P(), P(), P("tp", "fs"), P(),
    )
    return jax.shard_map(shards, mesh=mesh, in_specs=in_specs, out_specs=P(("rep", "fs", "tp"), None), check_vma=False)
```

```python
import functools

import jax
import jax.numpy as jnp
from jax import lax
from jax.experimental import pallas as pl
from jax.experimental.pallas import tpu as pltpu
from jax.sharding import PartitionSpec as P

MESH = pl.DeviceIdType.MESH
pool_spans = (2, 4, 8, 16)
rms_eps = 1e-06
weight_budget = 24 * 2**20
f32 = jnp.float32
bf16 = jnp.bfloat16


def rms_scale(floats, gain):
    return floats * lax.rsqrt(jnp.mean(floats * floats, axis=-1, keepdims=True) + rms_eps) * gain


def gelu(v):
    return 0.5 * v * (1.0 + jnp.tanh(0.7978845608028654 * (v + 0.044715 * v * v * v)))


class Plan:
    def __init__(self, mesh, depth, width, columns):
        self.R, self.F, self.T = mesh.shape["rep"], mesh.shape["fs"], mesh.shape["tp"]
        self.Y = 1
        while 4 * self.Y * self.Y <= self.F:
            self.Y *= 2
        while self.F % self.Y:
            self.Y -= 1
        self.Z = self.F // self.Y
        self.joined = 3 * width * columns * 2 > weight_budget
        self.n_sub = self.R * self.Y if self.joined else 1
        self.G = self.T * self.n_sub
        self.cols = columns // self.n_sub


def kernel(
    plan, tokens, gain_in, pool, gain_out, gain_ffn, gate_t, up_t, down_w, gate_taps, up_taps, gain_last, out,
    halo, pool_all, w_gu, w_d, x_all, normed, after, acc_g, acc_u, hidden, partial, swapped, summed, got,
    own_sem, halo_sem, y_ss, up_ss, dn_ss, piece_rs, share_ss, share_rs, x_ss, x_rs, f_ss, s_ss, s_rs, p_ss, p_rs,
):
    R, F, T, Y, Z, G, cols = plan.R, plan.F, plan.T, plan.Y, plan.Z, plan.G, plan.cols
    r, f, t = lax.axis_index("rep"), lax.axis_index("fs"), lax.axis_index("tp")
    z, y = f // Y, f % Y
    rows, width = tokens.shape
    depth = width // F
    groups, gc = pool_all.shape[0], pool_all.shape[1]
    slab = gc // F
    S = min(T, groups)
    GS = groups // S
    q = t % S
    margin = halo.shape[0]
    C = G // T
    POOL, GA, UP, DN = 0, 1, 2, 3
    kinds = (POOL, GA, UP, DN)
    GU = (GA, UP)

    chip = r * Y + y if plan.joined else 0
    me = chip * T + t

    def peer(step):
        to = (chip + step) % C
        return {"rep": to // Y, "fs": z * Y + to % Y}

    def sub_of(y_to):
        return r * Y + y_to if plan.joined else 0

    def w_rows(y_to):
        return pl.ds(pl.multiple_of(sub_of(y_to) * cols, 64 if cols % 64 == 0 else 8), cols)

    def slot(kind, origin):
        if kind == POOL:
            return pool_all.at[pl.ds(q * GS, GS), pl.ds(pl.multiple_of(origin * slab, slab), slab)]
        return w_d.at[origin] if kind == DN else w_gu.at[origin, kind - GA]

    def source(kind, y_to):
        if kind == POOL:
            return pool.at[pl.ds(q * GS, GS)]
        return (gate_t, up_t, down_w)[kind - GA].at[w_rows(y_to)]

    def own_copy(kind):
        return pltpu.make_async_copy(source(kind, y), slot(kind, f), own_sem.at[kind])

    def y_copy(kind, step):
        y_to = (y + step) % Y
        return pltpu.make_async_remote_copy(
            src_ref=source(kind, y_to), dst_ref=slot(kind, f), send_sem=y_ss.at[kind, step - 1],
            recv_sem=piece_rs.at[kind, f], device_id={"fs": z * Y + y_to}, device_id_type=MESH)

    def chain_copy(kind, origin, dz):
        return pltpu.make_async_remote_copy(
            src_ref=slot(kind, origin), dst_ref=slot(kind, origin), send_sem=(up_ss if dz > 0 else dn_ss).at[kind, origin],
            recv_sem=piece_rs.at[kind, origin], device_id={"fs": (z + dz) * Y + y}, device_id_type=MESH)

    def arrived(kind, origin):
        chain_copy(kind, origin, 1).wait_recv()

    def pass_on(kind, origin, z0):
        @pl.when((z0 <= z) & (z + 1 < Z))
        def _():
            chain_copy(kind, origin, 1).start()

        @pl.when((z0 >= z) & (z > 0))
        def _():
            chain_copy(kind, origin, -1).start()

    side = jnp.minimum(z, Z - 1 - z)

    def place(k):
        j = k // Y
        near = jnp.where(j % 2 == 1, z - (j + 1) // 2, z + j // 2)
        far = jnp.where(2 * z <= Z - 1, j, Z - 1 - j)
        z0 = jnp.where(j <= 2 * side, near, far)
        return z0, z0 * Y + (y + k % Y) % Y

    def chain(kinds_now, k):
        z0, origin = place(k)
        for kind in kinds_now:
            arrived(kind, origin)
            pass_on(kind, origin, z0)

    def chain_own(kinds_now):
        for kind in kinds_now:
            own_copy(kind).wait()
            pass_on(kind, f, z)

    def chain_range(kinds_now, first, last):
        def body(k, carry):
            chain(kinds_now, k)
            return carry
        lax.fori_loop(first, last, body, 0)

    def halo_copy():
        return pltpu.make_async_remote_copy(
            src_ref=tokens.at[pl.ds(rows - margin, margin)], dst_ref=halo, send_sem=halo_sem.at[0],
            recv_sem=halo_sem.at[1], device_id={"tp": (t + 1) % T}, device_id_type=MESH)

    def share_copy(step, q_from):
        return pltpu.make_async_remote_copy(
            src_ref=pool_all.at[pl.ds(q_from * GS, GS)], dst_ref=pool_all.at[pl.ds(q_from * GS, GS)],
            send_sem=share_ss.at[step - 1], recv_sem=share_rs.at[q_from],
            device_id={"tp": t - q + (q + step) % S}, device_id_type=MESH)

    def x_copy(step, c_from):
        g = c_from * T + t
        return pltpu.make_async_remote_copy(
            src_ref=x_all.at[g], dst_ref=x_all.at[g], send_sem=x_ss.at[step - 1],
            recv_sem=x_rs.at[g], device_id=peer(step), device_id_type=MESH)

    def x_across(step, c, t_from):
        g = c * T + t_from
        return pltpu.make_async_remote_copy(
            src_ref=x_all.at[g], dst_ref=x_all.at[g], send_sem=f_ss.at[step - 1, c],
            recv_sem=x_rs.at[g], device_id={"tp": (t + step) % T}, device_id_type=MESH)

    def s_copy(step, block, t_from):
        t_to = (t + step) % T
        return pltpu.make_async_remote_copy(
            src_ref=partial.at[block, t_to], dst_ref=swapped.at[block, t_from], send_sem=s_ss.at[block, step - 1],
            recv_sem=s_rs.at[block, t_from], device_id={"tp": t_to}, device_id_type=MESH)

    def p_copy(step, block, c_from):
        return pltpu.make_async_remote_copy(
            src_ref=summed.at[block, (chip + step) % C], dst_ref=got.at[block, c_from], send_sem=p_ss.at[block, step - 1],
            recv_sem=p_rs.at[block, c_from], device_id=peer(step), device_id_type=MESH)

    for kind in kinds:
        own_copy(kind).start()
    halo_copy().start()
    for kind in kinds:
        for step in range(1, Y):
            y_copy(kind, step).start()
    chain_own((POOL,))
    chain_own(GU)
    chain_range((POOL,), 1, F)
    chain_range(GU, 1, Y)
    for step in range(1, S):
        share_copy(step, q).start()

    halo_copy().wait_recv()
    before = rms_scale(halo[...].astype(f32), gain_in[...]).astype(bf16).astype(f32)
    normed[pl.ds(0, margin), :] = jnp.where(t > 0, before, 0.0)
    normed[pl.ds(margin, rows), :] = rms_scale(tokens[...].astype(f32), gain_in[...]).astype(bf16).astype(f32)
    where = t * rows + lax.broadcasted_iota(jnp.int32, (rows, gc), 0)
    for step in range(1, S):
        share_copy(step, (q + step) % S).wait_recv()
    for group, span in enumerate(pool_spans):
        total = normed[:, group * gc : (group + 1) * gc]
        block = total[margin:]
        reach = 1
        while reach < span:
            total = total + pltpu.roll(total, reach, 0)
            reach *= 2
        gap = (total[margin:] / jnp.minimum(where + 1, span).astype(f32) - block).astype(bf16)
        mixed = jnp.dot(gap, pool_all[group], preferred_element_type=f32)
        after[:, group * gc : (group + 1) * gc] = mixed.astype(bf16).astype(f32)
    after[...] = tokens[...].astype(f32) + rms_scale(after[...], gain_out[...])
    whole = rms_scale(after[...], gain_ffn[...]).astype(bf16)
    for k in range(F):
        x_all[me, k] = whole[:, k * depth : (k + 1) * depth]
    for step in range(1, C):
        x_copy(step, chip).start()
    for step in range(1, T):
        x_across(step, chip, t).start()

    acc_g[...] = jnp.zeros_like(acc_g)
    acc_u[...] = jnp.zeros_like(acc_u)

    def times(lhs, rhs):
        return lax.dot_general(lhs, rhs, (((1,), (1,)), ((), ())), preferred_element_type=f32)

    def gate_up(origin):
        def body(g, carry):
            x = x_all[g, origin]
            at = pl.ds(pl.multiple_of(8 + g * rows, 8), rows)
            acc_g[at, :] += times(x, w_gu[origin, 0])
            acc_u[at, :] += times(x, w_gu[origin, 1])
            return carry
        lax.fori_loop(0, G, body, 0)

    ahead = Y * (1 + jnp.maximum(1, 2 * side))
    chain_range(GU, Y, ahead)
    chain_own((DN,))
    chain_range((DN,), 1, Y)
    for back in range(1, C):
        c = (chip + C - back) % C
        x_copy(back, c).wait_recv()
        for step in range(1, T):
            x_across(step, c, t).start()
    for c in range(C):
        for step in range(1, T):
            x_across(step, c, (t + step) % T).wait_recv()

    def gate_up_step(k, carry):
        @pl.when(k >= ahead)
        def _():
            chain(GU, k)
        gate_up(place(k)[1])
        return carry
    lax.fori_loop(0, F, gate_up_step, 0)
    chain_range((DN,), Y, ahead)

    taps = gate_taps.shape[0]

    def convolve(acc, taps_ref, g, keep):
        block = acc[pl.ds(pl.multiple_of(g * rows, 8), rows + 8), :]
        total = taps_ref[taps - 1 : taps, :] * block[8:]
        for back in range(1, taps):
            moved = pltpu.roll(block, back, 0)[8:]
            total = total + taps_ref[taps - 1 - back : taps - back, :] * jnp.where(keep >= back, moved, 0.0)
        return total

    def activate(g, carry):
        keep = (g % T) * rows + lax.broadcasted_iota(jnp.int32, (rows, cols), 0)
        hidden[g] = (gelu(convolve(acc_g, gate_taps, g, keep)) * convolve(acc_u, up_taps, g, keep)).astype(bf16)
        return carry

    lax.fori_loop(0, G, activate, 0)

    def down(block):
        def body(i, carry):
            step, c = i // C + 1, i % C
            t_to = (t + step) % T
            product = jnp.dot(hidden[c * T + t_to], w_d[block], preferred_element_type=f32)
            partial[block, t_to, c] = product.astype(bf16)
            return carry
        lax.fori_loop(0, G - C, body, 0)
        for step in range(1, T):
            s_copy(step, block, t).start()
        lax.fori_loop(G - C, G, body, 0)

    def add_up(block):
        for back in range(1, T):
            s_copy(back, block, (t + back) % T).wait_recv()

        def body(c, carry):
            total = partial[block, t, c].astype(f32)
            for back in range(1, T):
                total = total + swapped[block, (t + back) % T, c].astype(f32)
            summed[block, c] = total.astype(bf16)
            return carry
        lax.fori_loop(0, C, body, 0)
        for step in range(1, C):
            p_copy(step, block, chip).start()
        got[block, chip] = summed[block, chip]

    def down_step(k, carry):
        @pl.when(k >= ahead)
        def _():
            chain((DN,), k)
        down(place(k)[1])

        @pl.when(k > 0)
        def _():
            add_up(place(k - 1)[1])
        return carry
    lax.fori_loop(0, F, down_step, 0)
    add_up(place(F - 1)[1])

    def finish(block, carry):
        for step in range(1, C):
            p_copy(step, block, (chip + step) % C).wait_recv()
        return carry

    lax.fori_loop(0, F, finish, 0)
    for k in range(F):
        total = got[k, 0].astype(f32)
        for c in range(1, C):
            total = total + got[k, c].astype(f32)
        normed[pl.ds(0, rows), k * depth : (k + 1) * depth] = total
    out[...] = (after[...] + rms_scale(normed[pl.ds(0, rows), :], gain_last[...])).astype(bf16)

    halo_copy().wait_send()
    for step in range(1, S):
        share_copy(step, q).wait_send()
    for step in range(1, C):
        x_copy(step, chip).wait_send()
    for step in range(1, T):
        for c in range(C):
            x_across(step, c, t).wait_send()
    for kind in kinds:
        for step in range(1, Y):
            y_copy(kind, step).wait_send()

        def ended(origin, carry):
            @pl.when((origin // Y <= z) & (z + 1 < Z))
            def _():
                chain_copy(kind, origin, 1).wait_send()

            @pl.when((origin // Y >= z) & (z > 0))
            def _():
                chain_copy(kind, origin, -1).wait_send()
            return carry
        lax.fori_loop(0, F, ended, 0)

    def sent(block, carry):
        for step in range(1, T):
            s_copy(step, block, t).wait_send()
        for step in range(1, C):
            p_copy(step, block, chip).wait_send()
        return carry
    lax.fori_loop(0, F, sent, 0)


def solution(mesh):
    def shards(tokens, gain_in, pool, gain_out, gain_ffn, gate_w, up_w, gate_taps, up_taps, down_w, gain_last):
        rows, width = tokens.shape
        depth, columns = gate_w.shape
        plan = Plan(mesh, depth, width, columns)
        F, G, T, Y, Z, cols = plan.F, plan.G, plan.T, plan.Y, plan.Z, plan.cols
        groups, gc = pool.shape[0], pool.shape[2]
        C = G // T
        first = lax.axis_index("tp") * columns
        if plan.joined:
            first = first + (lax.axis_index("rep") * Y + lax.axis_index("fs") % Y) * cols
        gt = lax.dynamic_slice_in_dim(gate_taps, first, cols, 1)
        ut = lax.dynamic_slice_in_dim(up_taps, first, cols, 1)
        margin = max(pool_spans)
        vmem = pl.BlockSpec(memory_space=pltpu.VMEM)
        anywhere = pl.BlockSpec(memory_space=pl.ANY)
        dma = pltpu.SemaphoreType.DMA
        S = min(T, groups)
        V = pltpu.VMEM
        return pl.pallas_call(
            functools.partial(kernel, plan),
            out_shape=jax.ShapeDtypeStruct((rows, width), bf16),
            in_specs=[vmem, vmem, anywhere, vmem, vmem, anywhere, anywhere, anywhere, vmem, vmem, vmem],
            out_specs=vmem,
            scratch_shapes=[
                V((margin, width), bf16), V((groups, gc, gc), bf16), V((F, 2, cols, depth), bf16), V((F, cols, depth), bf16),
                V((G, F, rows, depth), bf16), V((margin + rows, width), f32), V((rows, width), f32),
                V((8 + G * rows, cols), f32), V((8 + G * rows, cols), f32), V((G, rows, cols), bf16),
                V((F, T, C, rows, depth), bf16), V((F, T, C, rows, depth), bf16), V((F, C, rows, depth), bf16), V((F, C, rows, depth), bf16),
                dma((4,)), dma((2,)), dma((4, max(Y - 1, 1))), dma((4, F)), dma((4, F)), dma((4, F)),
                dma((max(S - 1, 1),)), dma((S,)), dma((max(C - 1, 1),)), dma((G,)),
                dma((max(T - 1, 1), C)), dma((F, max(T - 1, 1))), dma((F, T)), dma((F, max(C - 1, 1))), dma((F, C)),
            ],
            compiler_params=pltpu.CompilerParams(has_side_effects=True, vmem_limit_bytes=61 * 2**20),
            name="layer",
        )(tokens, gain_in[None], pool, gain_out[None], gain_ffn[None], gate_w.T, up_w.T, down_w, gt, ut, gain_last[None])

    in_specs = (
        P(("rep", "fs", "tp"), None), P(), P(None, "fs", None), P(), P(),
        P("fs", "tp"), P("fs", "tp"), P(), P(), P("tp", "fs"), P(),
    )
    return jax.shard_map(shards, mesh=mesh, in_specs=in_specs, out_specs=P(("rep", "fs", "tp"), None), check_vma=False)
```
